32 devices in a mesh: grp: 2 (over y), sp: 4 (over z), tp: 4 (over x, core).
Axes of the slice: x: 2, y: 2, z: 4, core: 2. Of those that a mesh axis runs over, the one named last changes fastest.
Arguments:
- conv_input: bfloat16 [4096, 1024], P(('grp', 'sp'), 'tp'), parts along dimension 0, may hold values from -6 to 6
- pre_gate: bfloat16 [4096, 1024], P(('grp', 'sp'), 'tp'), parts along dimension 0, may hold values from -6 to 6
- post_gate: bfloat16 [4096, 1024], P(('grp', 'sp'), 'tp'), parts along dimension 0, may hold values from -6 to 6
- conv_taps: float32 [3, 1024], replicated, may hold values from -3.5 to 3.5
- out_proj: bfloat16 [1024, 2048], replicated, may hold values from -0.1875 to 0.1875
- residual_in: bfloat16 [4096, 2048], P(('grp', 'sp', 'tp')), parts along dimension 0, may hold values from -6 to 6
- norm_gain: float32 [2048], replicated, may hold values from 0.1 to 1.9
- routes: int32 [4096, 2], P(('grp', 'sp', 'tp')), parts along dimension 0, may hold values from 0 to 7, as said below
- route_weight: float32 [4096, 2], P(('grp', 'sp', 'tp')), parts along dimension 0, may hold values from 0.1 to 1
- w_gate: bfloat16 [8, 2048, 1024], P('sp', None, 'tp'), may hold values from -0.125 to 0.125
- w_up: bfloat16 [8, 2048, 1024], P('sp', None, 'tp'), may hold values from -0.125 to 0.125
- w_down: bfloat16 [8, 1024, 2048], P('sp', 'tp'), may hold values from -0.1875 to 0.1875
Outputs:
- layer_out: bfloat16 [4096, 2048], P(('grp', 'sp', 'tp')), parts along dimension 0
The draws below stay inside these ranges and needn't reach their ends.
There are 2 independent parts, one for each index of `grp`. The reference program is written for one: setup_inputs(seed, part) draws one part's arguments, and reference() takes and returns one part's arrays. A program takes and returns all parts, laid end to end along the dimension named above; an argument that names none is the same for every part. Nothing has to cross between parts.
Inputs may be any that keep to these rules, and one draw needn't show every extreme that they name: `routes`: the two numbers of a row differ and lie in the same group of 2 consecutive experts. In each aligned block of 128 rows every expert is named exactly 32 times.
All inputs are finite; a program needn't handle non-finite values.
Results may differ from the reference program's by a relative error of at most 0.0085.
Values may be sent and summed in bfloat16 or wider, within the bound.
No kernel may reach another device: no remote copies, remote signals or barrier semaphores. Data moves between devices by JAX's collectives and lax.ppermute only.
A program may use at most 64 MiB of HBM per device.

```python
import jax
import jax.numpy as jnp
from jax import lax

D = 2048
CH = 1024
HID = 1024
CONV = 3
GROUPS = 4
TOKENS = 2048
EXPERTS = 8
EPG = 2
ROW_BLOCK = 128
BLOCKS = 16
N_TP = 4


def draw_routes(key, part):
    base = jax.random.fold_in(key, 7)
    perm_key, shift_key = jax.random.split(base)
    block_keys = jax.random.split(perm_key, BLOCKS)
    ranks = jax.vmap(lambda k: jax.random.permutation(k, ROW_BLOCK))(block_keys).astype(jnp.int32)
    offsets = jax.random.randint(shift_key, (BLOCKS, 1), 0, EPG // 2).astype(jnp.int32)
    group = ranks % GROUPS
    within = ranks // GROUPS
    first = 2 * within % EPG
    second = (2 * within + 1 + 2 * offsets) % EPG
    chosen = jnp.stack([group * EPG + first, group * EPG + second], axis=-1)
    return chosen.reshape(TOKENS, 2).astype(jnp.int32)


def block_scale(own_key, shape, cuts, least, high):
    level = 1.0
    for position, shards_of in cuts:
        steps = jax.random.uniform(jax.random.fold_in(jax.random.fold_in(own_key, 6), position), (shards_of,), jnp.float32, least / len(cuts), high / len(cuts))
        level = level * jnp.repeat(jnp.exp(steps), shape[position] // shards_of).reshape((-1,) + (1,) * (len(shape) - 1 - position))
    return level


def gaussian(rng, dims, spread, most, pieces=(), held_as=jnp.bfloat16):
    entries = spread * jax.random.normal(rng, dims, jnp.float32)
    if pieces:
        entries = entries * block_scale(rng, dims, pieces, -0.22, 0.18)
    return jnp.clip(entries, -most, most).astype(held_as)


def setup_inputs(seed: int = 0, part: int = 0) -> dict:
    key_of = jax.random.split(jax.random.key(seed), 13)
    part_splits = jax.random.split(jax.random.fold_in(key_of[12], part), 13)
    conv_input = gaussian(part_splits[0], (TOKENS, CH), 1.0, 6.0, ((0, 4), (1, 4)))
    pre_gate = gaussian(part_splits[1], (TOKENS, CH), 1.0, 6.0, ((0, 4), (1, 4)))
    post_gate = gaussian(part_splits[2], (TOKENS, CH), 1.0, 6.0, ((0, 4), (1, 4)))
    conv_taps = gaussian(key_of[3], (CONV, CH), CONV ** -0.5, 3.5, (), jnp.float32)
    out_proj = gaussian(key_of[4], (CH, D), CH ** -0.5, 0.1875)
    residual_in = gaussian(part_splits[5], (TOKENS, D), 1.0, 6.0, ((0, 16),))
    norm_gain = jnp.clip(1.0 + 0.18 * jax.random.normal(key_of[6], (D,), jnp.float32), 0.1, 1.9)
    routes = draw_routes(jax.random.fold_in(jax.random.fold_in(key_of[12], part), 71), part)
    route_weight = jnp.clip(0.1 + 0.9 * jax.random.uniform(part_splits[8], (TOKENS, 2), jnp.float32) ** block_scale(part_splits[8], (TOKENS, 2), ((0, 16),), -0.2, 0.2), 0.1, 1.0)
    w_gate = gaussian(key_of[9], (EXPERTS, D, HID), D ** -0.5, 0.125, ((0, 4), (2, 4)))
    w_up = gaussian(key_of[10], (EXPERTS, D, HID), D ** -0.5, 0.125, ((0, 4), (2, 4)))
    w_down = gaussian(key_of[11], (EXPERTS, HID, D), HID ** -0.5, 0.1875, ((0, 4), (1, 4)))
    return dict(conv_input=conv_input, pre_gate=pre_gate, post_gate=post_gate, conv_taps=conv_taps, out_proj=out_proj, residual_in=residual_in, norm_gain=norm_gain, routes=routes, route_weight=route_weight, w_gate=w_gate, w_up=w_up, w_down=w_down)


def reference(conv_input, pre_gate, post_gate, conv_taps, out_proj, residual_in, norm_gain, routes, route_weight, w_gate, w_up, w_down):
    gated = pre_gate.astype(jnp.float32) * conv_input.astype(jnp.float32)
    padded = jnp.pad(gated, ((2, 0), (0, 0)))
    conv = padded[2:] * conv_taps[2] + padded[1:-1] * conv_taps[1] + padded[:-2] * conv_taps[0]
    mixed = (post_gate.astype(jnp.float32) * conv).astype(jnp.bfloat16)
    projected = jnp.dot(mixed, out_proj, preferred_element_type=jnp.float32)
    stream = residual_in.astype(jnp.float32) + projected
    scale = lax.rsqrt(lax.optimization_barrier(jnp.mean(stream * stream, axis=-1, keepdims=True)) + 1e-06)
    normed = (stream * scale * norm_gain).astype(jnp.bfloat16)
    flat_routes = routes.reshape(-1)
    per_expert = TOKENS * 2 // EXPERTS
    hid_shard = HID // N_TP

    def one_expert(carry, expert):
        picked = jnp.nonzero(flat_routes == expert, size=per_expert)[0].astype(jnp.int32)
        rows = normed[picked // 2]
        gate_all = w_gate[expert]
        up_all = w_up[expert]
        down_all = w_down[expert]
        total = jnp.zeros((per_expert, D), jnp.float32)
        for shard in range(N_TP):
            low = shard * hid_shard
            gate = jnp.dot(rows, gate_all[:, low:low + hid_shard], preferred_element_type=jnp.float32)
            upper = jnp.dot(rows, up_all[:, low:low + hid_shard], preferred_element_type=jnp.float32)
            hidden = (jax.nn.silu(gate) * upper).astype(jnp.bfloat16)
            part = jnp.dot(hidden, down_all[low:low + hid_shard], preferred_element_type=jnp.float32).astype(jnp.bfloat16)
            part = lax.optimization_barrier(part)
            total = total + part.astype(jnp.float32)
        carry = carry.at[picked].set(total.astype(jnp.bfloat16))
        return (carry, None)
    start = jnp.zeros((TOKENS * 2, D), jnp.bfloat16)
    outputs, _ = lax.scan(one_expert, start, jnp.arange(EXPERTS, dtype=jnp.int32))
    expert_out = outputs.reshape(TOKENS, 2, D).astype(jnp.float32)
    weighted = lax.optimization_barrier(jnp.sum(route_weight[:, :, None] * expert_out, axis=1))
    return (stream + weighted).astype(jnp.bfloat16)
```

```python
import jax
import jax.numpy as jnp
from jax import lax
from jax.sharding import PartitionSpec as P

GROUPS = 4
LANES = 128


def shifted(block, axis, distance):
    devices = range(lax.axis_size(axis))
    route = [(i - distance, i) for i in devices if i - distance in devices]
    return lax.ppermute(block, axis, route)


def flipped(block, axis, bit):
    return lax.ppermute(block, axis, [(i, i ^ bit) for i in range(lax.axis_size(axis))])


def mix(conv_input, pre_gate, post_gate, conv_taps):
    channels = conv_input.shape[1]
    taps = lax.dynamic_slice_in_dim(conv_taps, lax.axis_index("tp") * channels, channels, 1)
    edge = jnp.concatenate([conv_input[-2:], pre_gate[-2:]], axis=1)
    prior = shifted(edge, "sp", 1)
    prior_input, prior_gate = prior[:, :channels], prior[:, channels:]
    gated = jnp.concatenate(
        [
            prior_gate.astype(jnp.float32) * prior_input.astype(jnp.float32),
            pre_gate.astype(jnp.float32) * conv_input.astype(jnp.float32),
        ],
        axis=0,
    )
    conv = gated[2:] * taps[2] + gated[1:-1] * taps[1] + gated[:-2] * taps[0]
    return (post_gate.astype(jnp.float32) * conv).astype(jnp.bfloat16)


def project(mixed, out_proj, residual_in, norm_gain):
    token_rows = lax.all_to_all(mixed, "tp", split_axis=0, concat_axis=1, tiled=True)
    projected = jnp.dot(token_rows, out_proj, preferred_element_type=jnp.float32)
    stream = residual_in.astype(jnp.float32) + projected
    scale = lax.rsqrt(jnp.mean(stream * stream, axis=-1, keepdims=True) + 1e-06)
    normed = (stream * scale * norm_gain).astype(jnp.bfloat16)
    return stream, normed


def route_by_group(stream, normed, routes, route_weight, w_gate, w_up, w_down):
    shards = lax.axis_size("tp")
    seq_ranks = lax.axis_size("sp")
    block_rows, width = stream.shape
    local_experts = w_gate.shape[0]
    capacity = block_rows // seq_ranks
    group = routes[:, 0] // local_experts
    order = jnp.arange(block_rows, dtype=jnp.int32)
    earlier = (group[:, None] == group[None, :]) & (order[None, :] < order[:, None])
    slot = group * capacity + jnp.sum(earlier.astype(jnp.int32), axis=1)
    select = (order[:, None] == slot[None, :]).astype(jnp.bfloat16)
    member = routes[:, :, None] % local_experts == jnp.arange(local_experts, dtype=jnp.int32)
    weight = jnp.sum(jnp.where(member, route_weight[:, :, None], 0.0), axis=1)
    high = lax.reduce_precision(weight, 8, 7)
    labels = jnp.concatenate([high, weight - high], axis=1).astype(jnp.bfloat16)
    labels = jnp.pad(labels, ((0, 0), (0, LANES - labels.shape[1])))
    rows = jnp.concatenate([normed, labels], axis=1)
    outgoing = jnp.dot(select, rows, preferred_element_type=jnp.float32).astype(jnp.bfloat16)
    outgoing = outgoing.reshape(seq_ranks, capacity, width + LANES)
    arrived = lax.all_to_all(outgoing, "sp", split_axis=0, concat_axis=0, tiled=True)
    blocks = {0: arrived.reshape(block_rows, width + LANES)}
    bits = [1 << b for b in range(shards.bit_length() - 1)]
    for bit in reversed(bits):
        blocks.update({k | bit: flipped(v, "tp", bit) for k, v in blocks.items()})
    down = w_down.reshape(local_experts * w_down.shape[1], width)
    parts = {}
    for k, block in blocks.items():
        features = block[:, :width]
        marks = block[:, width:].astype(jnp.float32)
        hidden = []
        for expert in range(local_experts):
            gate = jnp.dot(features, w_gate[expert], preferred_element_type=jnp.float32)
            upper = jnp.dot(features, w_up[expert], preferred_element_type=jnp.float32)
            scale = marks[:, expert] + marks[:, local_experts + expert]
            hidden.append((jax.nn.silu(gate) * upper * scale[:, None]).astype(jnp.bfloat16))
        hidden = jnp.concatenate(hidden, axis=1)
        parts[k] = jnp.dot(hidden, down, preferred_element_type=jnp.float32)
    for bit in bits:
        for k in [k for k in parts if k & bit]:
            parts[k ^ bit] += flipped(parts.pop(k).astype(jnp.bfloat16), "tp", bit).astype(
                jnp.float32
            )
    summed = parts[0].astype(jnp.bfloat16).reshape(seq_ranks, capacity, width)
    returned = lax.all_to_all(summed, "sp", split_axis=0, concat_axis=0, tiled=True)
    weighted = lax.dot_general(
        select,
        returned.reshape(block_rows, width),
        (((0,), (0,)), ((), ())),
        preferred_element_type=jnp.float32,
    )
    return (stream + weighted).astype(jnp.bfloat16)


def route_by_expert(stream, normed, routes, route_weight, w_gate, w_up, w_down):
    shards = lax.axis_size("tp")
    seq_ranks = lax.axis_size("sp")
    block_rows, width = stream.shape
    local_experts = w_gate.shape[0]
    experts = local_experts * seq_ranks
    capacity = 2 * block_rows // experts
    flat_routes = routes.reshape(-1)
    position = jnp.arange(flat_routes.shape[0], dtype=jnp.int32)
    earlier = (flat_routes[:, None] == flat_routes[None, :]) & (
        position[None, :] < position[:, None]
    )
    rank = jnp.sum(earlier.astype(jnp.int32), axis=1)
    slot = flat_routes * capacity + rank
    outgoing = (
        jnp.zeros((experts * capacity, width), jnp.bfloat16).at[slot].set(normed[position // 2])
    )
    outgoing = outgoing.reshape(seq_ranks, local_experts, capacity, width)
    spread = lax.all_gather(
        lax.all_to_all(outgoing, "sp", split_axis=0, concat_axis=0, tiled=True)[:, None],
        "tp",
        axis=1,
        tiled=True,
    )
    count = spread.shape[3]
    partials = []
    for expert in range(local_experts):
        rows = spread[:, :, expert].reshape(seq_ranks * shards * count, width)
        gate = jnp.dot(rows, w_gate[expert], preferred_element_type=jnp.float32)
        upper = jnp.dot(rows, w_up[expert], preferred_element_type=jnp.float32)
        hidden = (jax.nn.silu(gate) * upper).astype(jnp.bfloat16)
        part = jnp.dot(hidden, w_down[expert], preferred_element_type=jnp.float32).astype(
            jnp.bfloat16
        )
        partials.append(part.reshape(seq_ranks, shards, count, width))
    stacked = jnp.stack(partials, axis=2)
    summed = lax.psum_scatter(stacked, "tp", scatter_dimension=1, tiled=True).astype(jnp.float32)
    returned = lax.all_to_all(
        summed[:, 0].astype(jnp.bfloat16), "sp", split_axis=0, concat_axis=0, tiled=True
    )
    results = returned.reshape(experts * capacity, width)[slot]
    results = results.reshape(block_rows, 2, width).astype(jnp.float32)
    weighted = jnp.sum(route_weight[:, :, None] * results, axis=1)
    return (stream + weighted).astype(jnp.bfloat16)


def on_device(
    conv_input,
    pre_gate,
    post_gate,
    conv_taps,
    out_proj,
    residual_in,
    norm_gain,
    routes,
    route_weight,
    w_gate,
    w_up,
    w_down,
):
    shards = lax.axis_size("tp")
    mixed = mix(conv_input, pre_gate, post_gate, conv_taps)
    stream, normed = project(mixed, out_proj, residual_in, norm_gain)
    whole_groups = lax.axis_size("sp") == GROUPS and shards & (shards - 1) == 0
    route = route_by_group if whole_groups else route_by_expert
    return route(stream, normed, routes, route_weight, w_gate, w_up, w_down)


def solution(mesh):
    return jax.shard_map(
        on_device,
        mesh=mesh,
        in_specs=(
            P(("grp", "sp"), "tp"),
            P(("grp", "sp"), "tp"),
            P(("grp", "sp"), "tp"),
            P(),
            P(),
            P(("grp", "sp", "tp"), None),
            P(),
            P(("grp", "sp", "tp"), None),
            P(("grp", "sp", "tp"), None),
            P("sp", None, "tp"),
            P("sp", None, "tp"),
            P("sp", "tp", None),
        ),
        out_specs=P(("grp", "sp", "tp"), None),
        check_vma=False,
    )
```
